128 devices in a mesh: tp: 16 (over z, x), dp: 8 (over y, core).
Axes of the slice: x: 4, y: 4, z: 4, core: 2. Of those that a mesh axis runs over, the one named last changes fastest.
Arguments:
- tokens: bfloat16 [256, 4096], P('tp', 'dp'), may hold values from -6 to 6
- query_weight: bfloat16 [2, 4096, 2048], P(None, 'dp', 'tp'), may hold values from -0.09375 to 0.09375
- key_weight: bfloat16 [2, 4096, 2048], P(None, 'dp', 'tp'), may hold values from -0.09375 to 0.09375
- value_weight: bfloat16 [2, 4096, 2048], P(None, 'dp', 'tp'), may hold values from -0.09375 to 0.09375
- outgate_weight: bfloat16 [2, 4096, 2048], P(None, 'dp', 'tp'), may hold values from -0.09375 to 0.09375
- igate_weight: bfloat16 [2, 4096, 16], replicated, may hold values from -0.09375 to 0.09375
- fgate_weight: bfloat16 [2, 4096, 16], replicated, may hold values from -0.09375 to 0.09375
- norm_gain: float32 [2, 4096], P(None, 'dp'), may hold values from 0.1 to 1.9
- head_gain: float32 [2, 2048], P(None, 'tp'), may hold values from 0.1 to 1.9
- proj_weight: bfloat16 [2, 2048, 4096], P(None, 'tp', 'dp'), may hold values from -0.125 to 0.125
- cell_state: float32 [2, 256, 16, 128, 128], P(None, 'dp', 'tp'), may hold values from -1.8 to 1.8
- normer_state: float32 [2, 256, 16, 128], P(None, 'dp', 'tp'), may hold values from -1.8 to 1.8
- stab_state: float32 [2, 256, 16], P(None, 'dp', 'tp'), may hold values from -4 to 4
Outputs:
- final_rows: bfloat16 [256, 4096], P('tp', 'dp')
- cell_out: float32 [2, 256, 16, 128, 128], P(None, 'dp', 'tp')
- normer_out: float32 [2, 256, 16, 128], P(None, 'dp', 'tp')
- stab_out: float32 [2, 256, 16], P(None, 'dp', 'tp')
The draws below stay inside these ranges and needn't reach their ends.
All inputs are finite; a program needn't handle non-finite values.
Results may differ from the reference program's by a relative error of at most 0.012.
The reference program's roundings to bfloat16 on the way count: a program that leaves them out, or rounds other values in their place, can miss the bound.
Values may be sent and summed in bfloat16 or wider, within the bound.
A program may use at most 64 MiB of HBM per device.

```python
import jax
import jax.numpy as jnp
from jax import lax

D = 4096
HEADS = 16
DH = 128
BLOCKS = 2
INNER = 2048
BATCH = 256


def block_levels(own_key, dims, shards, least, top_value):
    def one(axis_at, shards_of):
        draws = jax.random.uniform(jax.random.fold_in(jax.random.fold_in(own_key, 6), axis_at), (shards_of,), jnp.float32, least / len(shards), top_value / len(shards))
        return jnp.repeat(jnp.exp(draws), dims[axis_at] // shards_of).reshape((-1,) + (1,) * (len(dims) - axis_at - 1))

    gain = one(*shards[0])
    for cut in shards[1:]:
        gain = gain * one(*cut)
    return gain


def centred(key, extent, deviation, bound, split=(), held_as=jnp.bfloat16):
    entries = deviation * jax.random.normal(key, extent, jnp.float32)
    if split:
        entries = entries * block_levels(key, extent, split, -0.22, 0.18)
    return jnp.clip(entries, -bound, bound).astype(held_as)


def setup_inputs(seed: int = 0) -> dict:
    key_of = jax.random.split(jax.random.key(seed), 14)
    return {
        "tokens": centred(key_of[0], (BATCH, D), 1.0, 6.0, ((0, 16), (1, 8))),
        "query_weight": centred(key_of[1], (BLOCKS, D, INNER), D ** -0.5, 0.09375, ((1, 8), (2, 16))),
        "key_weight": centred(key_of[2], (BLOCKS, D, INNER), D ** -0.5, 0.09375, ((1, 8), (2, 16))),
        "value_weight": centred(key_of[3], (BLOCKS, D, INNER), D ** -0.5, 0.09375, ((1, 8), (2, 16))),
        "outgate_weight": centred(key_of[4], (BLOCKS, D, INNER), D ** -0.5, 0.09375, ((1, 8), (2, 16))),
        "igate_weight": centred(key_of[5], (BLOCKS, D, HEADS), D ** -0.5, 0.09375),
        "fgate_weight": centred(key_of[6], (BLOCKS, D, HEADS), D ** -0.5, 0.09375),
        "norm_gain": jnp.clip(1.0 + 0.18 * jax.random.normal(key_of[7], (BLOCKS, D), jnp.float32), 0.1, 1.9),
        "head_gain": jnp.clip(1.0 + 0.18 * jax.random.normal(key_of[8], (BLOCKS, INNER), jnp.float32), 0.1, 1.9),
        "proj_weight": centred(key_of[9], (BLOCKS, INNER, D), INNER ** -0.5, 0.125, ((1, 16), (2, 8))),
        "cell_state": centred(key_of[10], (BLOCKS, BATCH, HEADS, DH, DH), 0.3, 1.8, ((1, 8), (2, 16)), jnp.float32),
        "normer_state": centred(key_of[11], (BLOCKS, BATCH, HEADS, DH), 0.3, 1.8, ((1, 8), (2, 16)), jnp.float32),
        "stab_state": centred(key_of[12], (BLOCKS, BATCH, HEADS), 1.0, 4.0, ((1, 8), (2, 16)), jnp.float32),
    }


EPSILON = 1e-06

def reference(tokens, query_weight, key_weight, value_weight, outgate_weight, igate_weight, fgate_weight, norm_gain, head_gain, proj_weight, cell_state, normer_state, stab_state):
    current = tokens
    batch_rows = tokens.shape[0]
    cell_list = []
    normer_list = []
    stab_list = []
    for layer_num in range(BLOCKS):
        as_float = current.astype(jnp.float32)
        inv_rms = lax.rsqrt(lax.optimization_barrier(jnp.mean(as_float * as_float, axis=1, keepdims=True)) + EPSILON)
        scaled = (as_float * norm_gain[layer_num].astype(jnp.float32)).astype(jnp.bfloat16)

        def product(weight):
            return jnp.dot(scaled, weight, preferred_element_type=jnp.float32) * inv_rms
        query_rows = product(query_weight[layer_num]).reshape(batch_rows, HEADS, DH)
        key_rows = (product(key_weight[layer_num]) * DH ** (-0.5)).reshape(batch_rows, HEADS, DH)
        value_rows = product(value_weight[layer_num]).reshape(batch_rows, HEADS, DH)
        outgate = product(outgate_weight[layer_num])
        igate = product(igate_weight[layer_num])
        forget = jax.nn.log_sigmoid(product(fgate_weight[layer_num]))
        prev_stab = stab_state[layer_num]
        new_stab = jnp.maximum(forget + prev_stab, igate)
        keep_rate = jnp.exp(forget + prev_stab - new_stab)
        write_rate = jnp.exp(igate - new_stab)
        new_cell = keep_rate[..., None, None] * cell_state[layer_num] + write_rate[..., None, None] * value_rows[..., :, None] * key_rows[..., None, :]
        new_normer = keep_rate[..., None] * normer_state[layer_num] + write_rate[..., None] * key_rows
        numerator = jnp.einsum('bhvd,bhd->bhv', new_cell, query_rows, precision=lax.Precision.HIGHEST)
        denominator = jnp.maximum(jnp.abs(lax.optimization_barrier(jnp.sum(new_normer * query_rows, axis=-1))), 1.0)
        readout = numerator / denominator[..., None]
        normed = readout * lax.rsqrt(lax.optimization_barrier(jnp.mean(readout * readout, axis=-1, keepdims=True)) + EPSILON)
        normed = normed * head_gain[layer_num].reshape(HEADS, DH)
        gated_out = (jax.nn.sigmoid(outgate) * normed.reshape(batch_rows, HEADS * DH)).astype(jnp.bfloat16)
        current = jnp.dot(gated_out, proj_weight[layer_num], preferred_element_type=jnp.float32).astype(jnp.bfloat16)
        cell_list.append(new_cell)
        normer_list.append(new_normer)
        stab_list.append(new_stab)
    return (current, jnp.stack(cell_list), jnp.stack(normer_list), jnp.stack(stab_list))
```

```python
import functools

import jax
import jax.numpy as jnp
from jax import lax
from jax.experimental import pallas as pl
from jax.experimental.pallas import tpu as pltpu
from jax.sharding import PartitionSpec as P

D = 4096
EPSILON = 1e-06
NB = 2
TP = 16
DP = 8
ROWS = 256
DH = 128
SIDE = 4
COLS = 512
TROWS = ROWS // TP
DROWS = ROWS // DP
QKVO = 4 * DH
SEMS = 13
PIECES = 8

F32 = jnp.float32
BF16 = jnp.bfloat16


def ring_distance(step):
    return min(step, SIDE - step)


TP_STEPS = sorted(
    ((dz, dx) for dz in range(SIDE) for dx in range(SIDE) if (dz, dx) != (0, 0)),
    key=lambda s: -(ring_distance(s[0]) + ring_distance(s[1])),
)
DP_STEPS = sorted(
    ((dy, dc) for dy in range(SIDE) for dc in range(2) if (dy, dc) != (0, 0)),
    key=lambda s: -(2 * ring_distance(s[0]) + s[1]),
)


def dot_nt(a, b):
    return lax.dot_general(a, b, (((1,), (1,)), ((), ())), preferred_element_type=F32)


def mega(
    tok,
    qw,
    kw,
    vw,
    ow,
    igt,
    fgt,
    ngain,
    hgain,
    pw,
    cell,
    normer,
    stab,
    final_out,
    cell_out,
    normer_out,
    stab_out,
    g,
    w,
    gates,
    grow,
    pwv,
    ngv,
    hgv,
    n0v,
    m0v,
    cv,
    chl,
    scaled,
    dsend,
    drecv,
    ysend,
    yrecv,
    qs,
    wvt,
    gat,
    osend0,
    osend1,
    orecv0,
    orecv1,
    fin,
    n1v,
    m1v,
    lsem,
    wsem,
    ssem,
    rsem,
):
    me_t = lax.axis_index("tp")
    me_d = lax.axis_index("dp")
    z, x = me_t // SIDE, me_t % SIDE
    y, core = me_d // 2, me_d % 2
    tp_peers = [((z + dz) % SIDE) * SIDE + (x + dx) % SIDE for dz, dx in TP_STEPS]
    dp_peers = [((y + dy) % SIDE) * 2 + (core + dc) % 2 for dy, dc in DP_STEPS]
    y_peers = [(y + dy) % SIDE for dy in (2, 1, 3)]
    partner = y * 2 + 1 - core
    own_t = pl.ds(pl.multiple_of(me_t * TROWS, TROWS), TROWS)
    own_d = pl.ds(pl.multiple_of(me_d * DROWS, DROWS), DROWS)
    own_cols = pl.ds(pl.multiple_of(me_d * COLS, COLS), COLS)

    loads = [pltpu.make_async_copy(tok, g.at[0, own_t], lsem.at[0])]
    loads.append(pltpu.make_async_copy(ngain, ngv, lsem.at[1]))
    loads.append(pltpu.make_async_copy(igt.at[:, :, own_cols], gates.at[0], lsem.at[2]))
    loads.append(pltpu.make_async_copy(fgt.at[:, :, own_cols], gates.at[1], lsem.at[3]))
    for i, src in enumerate((qw, kw, vw, ow)):
        loads.append(
            pltpu.make_async_copy(src, w.at[:, :, pl.ds(i * DH, DH)], lsem.at[4 + i])
        )
    loads.append(pltpu.make_async_copy(pw, pwv, lsem.at[8]))
    loads.append(pltpu.make_async_copy(hgain, hgv, lsem.at[9]))
    loads.append(pltpu.make_async_copy(normer, n0v, lsem.at[10]))
    loads.append(pltpu.make_async_copy(stab, m0v, lsem.at[11]))
    loads.append(pltpu.make_async_copy(cell.at[0], cv.at[0], lsem.at[12]))
    loads.append(pltpu.make_async_copy(cell.at[1], cv.at[1], lsem.at[13]))
    for load in loads:
        load.start()

    barrier = pltpu.get_barrier_semaphore()
    for t in tp_peers:
        pl.semaphore_signal(barrier, inc=1, device_id={"tp": t})
    for d in dp_peers:
        pl.semaphore_signal(barrier, inc=1, device_id={"dp": d})
    loads[0].wait()
    pl.semaphore_wait(barrier, TP + DP - 2)

    def send(src, dst, sem, axis, peer):
        pltpu.make_async_remote_copy(
            src_ref=src,
            dst_ref=dst,
            send_sem=ssem.at[sem],
            recv_sem=rsem.at[sem],
            device_id={axis: peer},
        ).start()

    def wait_bytes(ref, sem):
        pltpu.make_async_copy(ref, ref, sem).wait()

    def gather_rows(b, sem):
        for t in tp_peers:
            send(g.at[b, own_t], g.at[b, own_t], sem, "tp", t)

    gather_rows(0, 0)

    for load in loads[1:12]:
        load.wait()
    row = lax.broadcasted_iota(jnp.int32, (DH, TP), 0)
    col = lax.broadcasted_iota(jnp.int32, (DH, TP), 1)
    for b in range(NB):
        picked = jnp.zeros((DH, COLS), F32)
        for i in range(2):
            onehot = jnp.where((row == i) & (col == me_t), 1.0, 0.0).astype(BF16)
            picked = picked + jnp.dot(onehot, gates[i, b], preferred_element_type=F32)
        grow[b] = picked.astype(BF16)
    for b in range(NB):
        loads[12 + b].wait()

        def split(s, carry):
            c0 = cv[b, s]
            hi = c0.astype(BF16)
            chl[b, s, 0:DH] = hi
            chl[b, s, DH : 2 * DH] = (c0 - hi.astype(F32)).astype(BF16)
            return carry

        lax.fori_loop(0, DROWS, split, 0)

    lane = lax.broadcasted_iota(jnp.int32, (DROWS, DH), 1)
    eye = lax.broadcasted_iota(jnp.int32, (DROWS, DROWS), 0) == lax.broadcasted_iota(
        jnp.int32, (DROWS, DROWS), 1
    )
    sub8 = lax.broadcasted_iota(jnp.int32, (8, DH), 0)
    lane_q = lax.broadcasted_iota(jnp.int32, (DH, DROWS), 1)
    half = SIDE * DROWS
    stores = []
    outs = ((osend0, orecv0), (osend1, orecv1))

    for b in range(NB):
        base = SEMS * b
        wait_bytes(g.at[b, pl.ds(0, ROWS - TROWS)], rsem.at[base])

        for h, c in ((0, 1 - core), (1, core)):
            squares = []
            for yy in range(SIDE):
                rows = pl.ds(pl.multiple_of((2 * yy + c) * DROWS, DROWS), DROWS)
                xf = g[b, rows].astype(F32)
                squares.append(jnp.sum(xf * xf, axis=1, keepdims=True))
                scaled[h, yy * DROWS : (yy + 1) * DROWS] = (
                    xf * ngv[pl.ds(b, 1), :]
                ).astype(BF16)
            dst = (dsend, ysend)[h]
            for i in range(2):
                two = jnp.dot(
                    scaled[h],
                    w[b, :, 2 * i * DH : 2 * (i + 1) * DH],
                    preferred_element_type=F32,
                )
                for n in range(2):
                    dst[b, 2 * i + n] = two[:, n * DH : (n + 1) * DH].reshape(
                        SIDE, DROWS, DH
                    )
                    if h == 0:
                        at = base + 1 + 2 * i + n
                        src = dsend.at[b, 2 * i + n]
                        send(src, drecv.at[b, 2 * i + n], at, "dp", partner)
            tail = dot_nt(scaled[h], grow[b])
            for yy in range(SIDE):
                dst[b, 4, yy] = jnp.where(
                    lane == 2, squares[yy], tail[yy * DROWS : (yy + 1) * DROWS]
                )
            if h == 0:
                send(dsend.at[b, 4], drecv.at[b, 4], base + 5, "dp", partner)

        for i in (0, 1, 2, 4, 3):
            wait_bytes(drecv.at[b, i], rsem.at[base + 1 + i])
            ysend[b, i] = ysend[b, i] + drecv[b, i]
            for yy in y_peers:
                send(
                    ysend.at[b, i, yy],
                    yrecv.at[b, i, y],
                    base + 6 + i,
                    "dp",
                    yy * 2 + core,
                )

        def arrived(i):
            wait_bytes(yrecv.at[b, i, pl.ds(0, SIDE - 1)], rsem.at[base + 6 + i])
            total = ysend[b, i, y]
            for yy in y_peers:
                total = total + yrecv[b, i, yy]
            return total

        query = arrived(0)
        q_hi = query.astype(BF16).astype(F32)
        q_lo = query - q_hi
        groups = []
        for j in range(DROWS // 8):
            rows = slice(8 * j, 8 * j + 8)
            qs[j] = jnp.concatenate([q_hi[rows], q_lo[rows]], axis=0).astype(BF16)
        for j in range(DROWS // 8):
            acc = jnp.zeros((8, DH), F32)
            for i in range(8):
                r = dot_nt(qs[j], chl[b, 8 * j + i])
                r = r[0:8, 0:DH] + (r[8:16, 0:DH] + r[0:8, DH : 2 * DH])
                acc = jnp.where(sub8 == i, r, acc)
            groups.append(acc)
        old_read = jnp.concatenate(groups, axis=0)

        key = arrived(1)
        value = arrived(2)
        tail = arrived(4)
        inv_rms = lax.rsqrt(tail[:, 2:3] * (1.0 / D) + EPSILON)
        query = query * inv_rms
        old_read = old_read * inv_rms
        key = key * (inv_rms * DH**-0.5)
        value = value * inv_rms
        igate = tail[:, 0:1] * inv_rms
        fpre = tail[:, 1:2] * inv_rms
        forget = jnp.minimum(fpre, 0.0) - jnp.log1p(jnp.exp(-jnp.abs(fpre)))
        prev = jnp.sum(jnp.where(eye, m0v[pl.ds(b, 1), :], 0.0), axis=1, keepdims=True)
        new_stab = jnp.maximum(forget + prev, igate)
        keep = jnp.exp(forget + prev - new_stab)
        write = jnp.exp(igate - new_stab)
        new_normer = keep * n0v[b] + write * key
        key_query = jnp.sum(key * query, axis=1, keepdims=True)
        numer = keep * old_read + (write * key_query) * value
        denom = jnp.maximum(
            jnp.abs(jnp.sum(new_normer * query, axis=1, keepdims=True)), 1.0
        )
        readout = numer / denom
        normed = readout * lax.rsqrt(
            jnp.mean(readout * readout, axis=1, keepdims=True) + EPSILON
        )
        normed = normed * hgv[pl.ds(b, 1), :]
        outgate = arrived(3) * inv_rms
        gat[b, own_d] = (normed / (1.0 + jnp.exp(-outgate))).astype(BF16)
        for d in dp_peers:
            send(gat.at[b, own_d], gat.at[b, own_d], base + 11, "dp", d)

        n1v[b] = new_normer
        m1v[pl.ds(b, 1), :] = jnp.sum(
            jnp.where(eye, new_stab, 0.0), axis=0, keepdims=True
        )
        wvt[0:DROWS] = jnp.broadcast_to(keep, (DROWS, DH))
        wvt[DROWS : 2 * DROWS] = key
        wv_cols = jnp.transpose(write * value)

        def update(s, carry):
            column = jnp.sum(
                jnp.where(lane_q == s, wv_cols, 0.0), axis=1, keepdims=True
            )
            k_row = wvt[pl.ds(DROWS + s, 1), :]
            keep_row = wvt[pl.ds(s, 1), :]
            cv[b, s] = keep_row * cv[b, s] + column * k_row
            return carry

        lax.fori_loop(0, DROWS, update, 0)
        stores.append(pltpu.make_async_copy(cv.at[b], cell_out.at[b], wsem.at[b]))
        stores[-1].start()

        wait_bytes(gat.at[b, pl.ds(0, ROWS - DROWS)], rsem.at[base + 11])
        osend, orecv = outs[b]
        osend[...] = jnp.dot(gat[b], pwv[b], preferred_element_type=F32).astype(
            osend.dtype
        )
        for t in tp_peers:
            rows = pl.ds(pl.multiple_of(t * TROWS, TROWS), TROWS)
            send(osend.at[rows], orecv.at[me_t], base + 12, "tp", t)
        orecv[me_t] = osend[own_t]
        wait_bytes(orecv.at[pl.ds(0, TP - 1)], rsem.at[base + 12])
        rows_sum = orecv[0].astype(F32)
        for i in range(1, TP):
            rows_sum = rows_sum + orecv[i].astype(F32)
        if b + 1 < NB:
            g[b + 1, own_t] = rows_sum.astype(BF16)
            gather_rows(b + 1, base + SEMS)
        else:
            fin[...] = rows_sum.astype(BF16)

    for i, (src, dst) in enumerate(
        ((fin, final_out), (n1v, normer_out), (m1v, stab_out))
    ):
        stores.append(pltpu.make_async_copy(src, dst, wsem.at[NB + i]))
        stores[-1].start()
    for b in range(NB):
        base = SEMS * b
        wait_bytes(g.at[b, pl.ds(0, ROWS - TROWS)], ssem.at[base])
        for i in range(5):
            wait_bytes(drecv.at[b, i], ssem.at[base + 1 + i])
            wait_bytes(yrecv.at[b, i, pl.ds(0, SIDE - 1)], ssem.at[base + 6 + i])
        wait_bytes(gat.at[b, pl.ds(0, ROWS - DROWS)], ssem.at[base + 11])
        wait_bytes(outs[b][1].at[pl.ds(0, TP - 1)], ssem.at[base + 12])
    for store in stores:
        store.wait()


def hand_on(final, cell, normer, stab, final_out, cell_out, normer_out, stab_out, *rest):
    fin, cv, n1v, m1v, sem_in, sem_out = rest
    pairs = []
    for b in range(NB):
        for i in range(PIECES):
            rows = pl.ds(i * (DROWS // PIECES), DROWS // PIECES)
            pairs.append((cell.at[b, rows], cv.at[b, rows], cell_out.at[b, rows]))
    pairs.append((final, fin, final_out))
    pairs.append((normer, n1v, normer_out))
    pairs.append((stab, m1v, stab_out))
    reads = [
        pltpu.make_async_copy(src, mid, sem_in.at[i])
        for i, (src, mid, _) in enumerate(pairs)
    ]
    writes = [
        pltpu.make_async_copy(mid, dst, sem_out.at[i])
        for i, (_, mid, dst) in enumerate(pairs)
    ]
    for read in reads:
        read.start()
    for read, write in zip(reads, writes):
        read.wait()
        write.start()
    for write in writes:
        write.wait()


def per_device(
    tokens,
    query_weight,
    key_weight,
    value_weight,
    outgate_weight,
    igate_weight,
    fgate_weight,
    norm_gain,
    head_gain,
    proj_weight,
    cell_state,
    normer_state,
    stab_state,
):
    anywhere = pl.BlockSpec(memory_space=pl.ANY)
    results = (
        jax.ShapeDtypeStruct((TROWS, COLS), BF16),
        jax.ShapeDtypeStruct((NB, DROWS, DH, DH), F32),
        jax.ShapeDtypeStruct((NB, DROWS, DH), F32),
        jax.ShapeDtypeStruct((NB, DROWS), F32),
    )
    held = pl.pallas_call(
        mega,
        out_shape=results,
        in_specs=[anywhere] * 13,
        out_specs=(anywhere,) * 4,
        scratch_shapes=[
            pltpu.VMEM((NB, ROWS, COLS), BF16),
            pltpu.VMEM((NB, COLS, QKVO), BF16),
            pltpu.VMEM((2, NB, TP, COLS), BF16),
            pltpu.VMEM((NB, DH, COLS), BF16),
            pltpu.VMEM((NB, DH, COLS), BF16),
            pltpu.VMEM((NB, COLS), F32),
            pltpu.VMEM((NB, DH), F32),
            pltpu.VMEM((NB, DROWS, DH), F32),
            pltpu.VMEM((NB, DROWS), F32),
            pltpu.VMEM((NB, DROWS, DH, DH), F32),
            pltpu.VMEM((NB, DROWS, 2 * DH, DH), BF16),
            pltpu.VMEM((2, SIDE * DROWS, COLS), BF16),
            pltpu.VMEM((NB, 5, SIDE, DROWS, DH), F32),
            pltpu.VMEM((NB, 5, SIDE, DROWS, DH), F32),
            pltpu.VMEM((NB, 5, SIDE, DROWS, DH), F32),
            pltpu.VMEM((NB, 5, SIDE, DROWS, DH), F32),
            pltpu.VMEM((DROWS // 8, 16, DH), BF16),
            pltpu.VMEM((2 * DROWS, DH), F32),
            pltpu.VMEM((NB, ROWS, DH), BF16),
            pltpu.VMEM((ROWS, COLS), F32),
            pltpu.VMEM((ROWS, COLS), BF16),
            pltpu.VMEM((TP, TROWS, COLS), F32),
            pltpu.VMEM((TP, TROWS, COLS), BF16),
            pltpu.VMEM((TROWS, COLS), BF16),
            pltpu.VMEM((NB, DROWS, DH), F32),
            pltpu.VMEM((NB, DROWS), F32),
            pltpu.SemaphoreType.DMA((14,)),
            pltpu.SemaphoreType.DMA((NB + 3,)),
            pltpu.SemaphoreType.DMA((SEMS * NB,)),
            pltpu.SemaphoreType.DMA((SEMS * NB,)),
        ],
        compiler_params=pltpu.CompilerParams(
            collective_id=0, has_side_effects=True, vmem_limit_bytes=60 * 10**6
        ),
        name="two_blocks",
    )(
        tokens,
        query_weight,
        key_weight,
        value_weight,
        outgate_weight,
        jnp.swapaxes(igate_weight, 1, 2),
        jnp.swapaxes(fgate_weight, 1, 2),
        norm_gain,
        head_gain,
        proj_weight,
        cell_state.reshape(NB, DROWS, DH, DH),
        normer_state.reshape(NB, DROWS, DH),
        stab_state.reshape(NB, DROWS),
    )
    moves = NB * PIECES + 3
    final_rows, cells, normers, stabs = pl.pallas_call(
        hand_on,
        out_shape=results,
        in_specs=[anywhere] * 4,
        out_specs=(anywhere,) * 4,
        scratch_shapes=[pltpu.VMEM(r.shape, r.dtype) for r in results]
        + [pltpu.SemaphoreType.DMA((moves,)), pltpu.SemaphoreType.DMA((moves,))],
        compiler_params=pltpu.CompilerParams(vmem_limit_bytes=60 * 10**6),
        name="hand_on",
    )(*held)
    return (
        final_rows,
        cells.reshape(cell_state.shape),
        normers.reshape(normer_state.shape),
        stabs.reshape(stab_state.shape),
    )


def solution(mesh):
    return jax.shard_map(
        per_device,
        mesh=mesh,
        in_specs=(
            P("tp", "dp"),
            P(None, "dp", "tp"),
            P(None, "dp", "tp"),
            P(None, "dp", "tp"),
            P(None, "dp", "tp"),
            P(),
            P(),
            P(None, "dp"),
            P(None, "tp"),
            P(None, "tp", "dp"),
            P(None, "dp", "tp", None, None),
            P(None, "dp", "tp", None),
            P(None, "dp", "tp"),
        ),
        out_specs=(
            P("tp", "dp"),
            P(None, "dp", "tp", None, None),
            P(None, "dp", "tp", None),
            P(None, "dp", "tp"),
        ),
        check_vma=False,
    )
```

```python
import functools

import jax
import jax.numpy as jnp
from jax import lax
from jax.experimental import pallas as pl
from jax.experimental.pallas import tpu as pltpu
from jax.sharding import PartitionSpec as P

D = 4096
EPSILON = 1e-06
NB = 2
TP = 16
DP = 8
ROWS = 256
DH = 128
SIDE = 4
COLS = 512
TROWS = ROWS // TP
DROWS = ROWS // DP
QKVO = 4 * DH
HALF = ROWS // 2
ROWS_SEM = 0
CORE_SEM = 1
CHIP_SEM = 6
GATED_SEM = 11
OUT_SEM = 15
SEMS = 16
ORDER = (0, 1, 4, 3, 2)
PIECES = 8

F32 = jnp.float32
BF16 = jnp.bfloat16


def ring_distance(step):
    return min(step, SIDE - step)


TP_STEPS = sorted(
    ((dz, dx) for dz in range(SIDE) for dx in range(SIDE) if (dz, dx) != (0, 0)),
    key=lambda s: -(ring_distance(s[0]) + ring_distance(s[1])),
)
DP_STEPS = sorted(
    ((dy, dc) for dy in range(SIDE) for dc in range(2) if (dy, dc) != (0, 0)),
    key=lambda s: -(2 * ring_distance(s[0]) + s[1]),
)


def dot_nt(a, b):
    return lax.dot_general(a, b, (((1,), (1,)), ((), ())), preferred_element_type=F32)


def mega(
    tok,
    qw,
    kw,
    vw,
    ow,
    igt,
    fgt,
    ngain,
    hgain,
    pw,
    cell,
    normer,
    stab,
    final_out,
    cell_out,
    normer_out,
    stab_out,
    g,
    w,
    gates,
    grow,
    pwv,
    ngv,
    hgv,
    n0v,
    m0v,
    cv,
    chl,
    scaled,
    dsend,
    drecv,
    ysend,
    yrecv,
    tsend,
    trecv,
    tysend,
    tyrecv,
    qs,
    wvt,
    gat,
    osend0,
    osend1,
    orecv0,
    orecv1,
    fin,
    n1v,
    m1v,
    lsem,
    wsem,
    ssem,
    rsem,
):
    me_t = lax.axis_index("tp")
    me_d = lax.axis_index("dp")
    z, x = me_t // SIDE, me_t % SIDE
    y, core = me_d // 2, me_d % 2
    tp_peers = [((z + dz) % SIDE) * SIDE + (x + dx) % SIDE for dz, dx in TP_STEPS]
    dp_peers = [((y + dy) % SIDE) * 2 + (core + dc) % 2 for dy, dc in DP_STEPS]
    y_peers = [(y + dy) % SIDE for dy in (2, 1, 3)]
    partner = y * 2 + 1 - core
    own_t = pl.ds(pl.multiple_of(me_t * TROWS, TROWS), TROWS)
    own_d = pl.ds(pl.multiple_of(me_d * DROWS, DROWS), DROWS)
    own_cols = pl.ds(pl.multiple_of(me_d * COLS, COLS), COLS)

    loads = [pltpu.make_async_copy(tok, g.at[0, own_t], lsem.at[0])]
    loads.append(pltpu.make_async_copy(ngain, ngv, lsem.at[1]))
    loads.append(pltpu.make_async_copy(igt.at[:, :, own_cols], gates.at[0], lsem.at[2]))
    loads.append(pltpu.make_async_copy(fgt.at[:, :, own_cols], gates.at[1], lsem.at[3]))
    for i, src in enumerate((qw, kw, vw, ow)):
        loads.append(
            pltpu.make_async_copy(src, w.at[:, :, pl.ds(i * DH, DH)], lsem.at[4 + i])
        )
    loads.append(pltpu.make_async_copy(pw, pwv, lsem.at[8]))
    loads.append(pltpu.make_async_copy(hgain, hgv, lsem.at[9]))
    loads.append(pltpu.make_async_copy(normer, n0v, lsem.at[10]))
    loads.append(pltpu.make_async_copy(stab, m0v, lsem.at[11]))
    loads.append(pltpu.make_async_copy(cell.at[0], cv.at[0], lsem.at[12]))
    loads.append(pltpu.make_async_copy(cell.at[1], cv.at[1], lsem.at[13]))
    for load in loads:
        load.start()

    barrier = pltpu.get_barrier_semaphore()
    for t in tp_peers:
        pl.semaphore_signal(barrier, inc=1, device_id={"tp": t})
    for d in dp_peers:
        pl.semaphore_signal(barrier, inc=1, device_id={"dp": d})
    loads[0].wait()
    pl.semaphore_wait(barrier, TP + DP - 2)

    def send(src, dst, sem, axis, peer):
        pltpu.make_async_remote_copy(
            src_ref=src,
            dst_ref=dst,
            send_sem=ssem.at[sem],
            recv_sem=rsem.at[sem],
            device_id={axis: peer},
        ).start()

    def wait_bytes(ref, sem):
        pltpu.make_async_copy(ref, ref, sem).wait()

    def gather_rows(b, sem):
        for t in tp_peers:
            send(g.at[b, own_t], g.at[b, own_t], sem, "tp", t)

    gather_rows(0, 0)

    for load in loads[1:12]:
        load.wait()
    row = lax.broadcasted_iota(jnp.int32, (TP, TP), 0)
    col = lax.broadcasted_iota(jnp.int32, (TP, TP), 1)
    for b in range(NB):
        picked = jnp.zeros((TP, COLS), F32)
        for i in range(2):
            onehot = jnp.where((row == i) & (col == me_t), 1.0, 0.0).astype(BF16)
            picked = picked + jnp.dot(onehot, gates[i, b], preferred_element_type=F32)
        grow[b] = picked.astype(BF16)
    for b in range(NB):
        loads[12 + b].wait()

        def split(s, carry):
            c0 = cv[b, s]
            hi = c0.astype(BF16)
            chl[b, s, 0:DH] = hi
            chl[b, s, DH : 2 * DH] = (c0 - hi.astype(F32)).astype(BF16)
            return carry

        lax.fori_loop(0, DROWS, split, 0)

    eye = lax.broadcasted_iota(jnp.int32, (DROWS, DROWS), 0) == lax.broadcasted_iota(
        jnp.int32, (DROWS, DROWS), 1
    )
    eye_wide = lax.broadcasted_iota(jnp.int32, (HALF, HALF), 0) == lax.broadcasted_iota(
        jnp.int32, (HALF, HALF), 1
    )
    own_lane = (
        lax.broadcasted_iota(jnp.int32, (DROWS, HALF), 0) + y * DROWS
    ) == lax.broadcasted_iota(jnp.int32, (DROWS, HALF), 1)
    sub8 = lax.broadcasted_iota(jnp.int32, (8, DH), 0)
    lane_q = lax.broadcasted_iota(jnp.int32, (DH, DROWS), 1)
    stores = []
    outs = ((osend0, orecv0), (osend1, orecv1))

    for b in range(NB):
        base = SEMS * b
        wait_bytes(g.at[b, pl.ds(0, ROWS - TROWS)], rsem.at[base + ROWS_SEM])

        sums = []
        for h, c in ((0, 1 - core), (1, core)):
            squares = []
            for yy in range(SIDE):
                rows = pl.ds(pl.multiple_of((2 * yy + c) * DROWS, DROWS), DROWS)
                xf = g[b, rows].astype(F32)
                squares.append(jnp.sum(xf * xf, axis=1, keepdims=True))
                at = h * HALF + yy * DROWS
                scaled[at : at + DROWS] = (xf * ngv[pl.ds(b, 1), :]).astype(BF16)
            sums.append(jnp.concatenate(squares, axis=0))

        def to_partner(i):
            if i < 4:
                src, dst = dsend.at[b, i], drecv.at[b, i]
            else:
                src, dst = tsend.at[b], trecv.at[b]
            send(src, dst, base + CORE_SEM + i, "dp", partner)

        def project(i):
            two = jnp.dot(
                scaled[...],
                w[b, :, 2 * i * DH : 2 * (i + 1) * DH],
                preferred_element_type=F32,
            )
            for n in range(2):
                tile = two[:, n * DH : (n + 1) * DH]
                dsend[b, 2 * i + n] = tile[0:HALF].reshape(SIDE, DROWS, DH)
                ysend[b, 2 * i + n] = tile[HALF:].reshape(SIDE, DROWS, DH)

        project(0)
        to_partner(0)
        to_partner(1)
        tail = dot_nt(grow[b], scaled[...])
        for h, dst in ((0, tsend), (1, tysend)):
            row_sums = jnp.sum(jnp.where(eye_wide, sums[h], 0.0), axis=0, keepdims=True)
            dst[b] = jnp.where(sub8 == 2, row_sums, tail[0:8, h * HALF : (h + 1) * HALF])
        to_partner(4)
        project(1)
        to_partner(3)
        to_partner(2)

        for i in ORDER:
            at = base + CHIP_SEM + i
            if i < 4:
                wait_bytes(drecv.at[b, i], rsem.at[base + CORE_SEM + i])
                ysend[b, i] = ysend[b, i] + drecv[b, i]
            else:
                wait_bytes(trecv.at[b], rsem.at[base + CORE_SEM + i])
                tysend[b] = tysend[b] + trecv[b]
            for yy in y_peers:
                if i < 4:
                    src, dst = ysend.at[b, i, yy], yrecv.at[b, i, y]
                else:
                    src, dst = tysend.at[b], tyrecv.at[b, y]
                send(src, dst, at, "dp", yy * 2 + core)

        def arrived(i):
            wait_bytes(yrecv.at[b, i, pl.ds(0, SIDE - 1)], rsem.at[base + CHIP_SEM + i])
            total = ysend[b, i, y]
            for yy in y_peers:
                total = total + yrecv[b, i, yy]
            return total

        query = arrived(0)
        q_hi = query.astype(BF16).astype(F32)
        q_lo = query - q_hi
        groups = []
        for j in range(DROWS // 8):
            rows = slice(8 * j, 8 * j + 8)
            qs[j] = jnp.concatenate([q_hi[rows], q_lo[rows]], axis=0).astype(BF16)
        for j in range(DROWS // 8):
            acc = jnp.zeros((8, DH), F32)
            for i in range(8):
                r = dot_nt(qs[j], chl[b, 8 * j + i])
                r = r[0:8, 0:DH] + (r[8:16, 0:DH] + r[0:8, DH : 2 * DH])
                acc = jnp.where(sub8 == i, r, acc)
            groups.append(acc)
        old_read = jnp.concatenate(groups, axis=0)

        key = arrived(1)
        wait_bytes(tyrecv.at[b, pl.ds(0, SIDE - 1)], rsem.at[base + CHIP_SEM + 4])
        tail = tysend[b]
        for yy in y_peers:
            tail = tail + tyrecv[b, yy]

        def column(i):
            return jnp.sum(
                jnp.where(own_lane, tail[i : i + 1], 0.0), axis=1, keepdims=True
            )

        inv_rms = lax.rsqrt(column(2) * (1.0 / D) + EPSILON)
        query = query * inv_rms
        old_read = old_read * inv_rms
        key = key * (inv_rms * DH**-0.5)
        igate = column(0) * inv_rms
        fpre = column(1) * inv_rms
        forget = jnp.minimum(fpre, 0.0) - jnp.log1p(jnp.exp(-jnp.abs(fpre)))
        prev = jnp.sum(jnp.where(eye, m0v[pl.ds(b, 1), :], 0.0), axis=1, keepdims=True)
        new_stab = jnp.maximum(forget + prev, igate)
        keep = jnp.exp(forget + prev - new_stab)
        write = jnp.exp(igate - new_stab)
        new_normer = keep * n0v[b] + write * key
        key_query = jnp.sum(key * query, axis=1, keepdims=True)
        denom = jnp.maximum(
            jnp.abs(jnp.sum(new_normer * query, axis=1, keepdims=True)), 1.0
        )
        outgate = arrived(3) * inv_rms
        scale = hgv[pl.ds(b, 1), :] / (1.0 + jnp.exp(-outgate))
        value = arrived(2) * inv_rms
        numer = keep * old_read + (write * key_query) * value
        readout = numer / denom
        normed = readout * lax.rsqrt(
            jnp.mean(readout * readout, axis=1, keepdims=True) + EPSILON
        )
        gat[b, own_d] = (normed * scale).astype(BF16)
        for dy, dc in DP_STEPS:
            peer = ((y + dy) % SIDE) * 2 + (core + dc) % 2
            at = base + GATED_SEM + (SIDE - dy) % SIDE
            send(gat.at[b, own_d], gat.at[b, own_d], at, "dp", peer)

        osend, orecv = outs[b]
        for dy in (0, 1, 3, 2):
            yy = (y + dy) % SIDE
            pieces = gat.at[b, pl.ds(0, DROWS if dy == 0 else 2 * DROWS)]
            wait_bytes(pieces, rsem.at[base + GATED_SEM + dy])
            rows = pl.ds(pl.multiple_of(yy * 2 * DROWS, 2 * DROWS), 2 * DROWS)
            osend[rows] = jnp.dot(
                gat[b, rows], pwv[b], preferred_element_type=F32
            ).astype(osend.dtype)

            def give(t):
                src = osend.at[pl.ds(pl.multiple_of(t * TROWS, TROWS), TROWS)]
                send(src, orecv.at[me_t], base + OUT_SEM, "tp", t)

            for dx in (2, 1, 3):
                give(yy * SIDE + (x + dx) % SIDE)

            @pl.when(yy != z)
            def _():
                give(yy * SIDE + x)

        n1v[b] = new_normer
        m1v[pl.ds(b, 1), :] = jnp.sum(
            jnp.where(eye, new_stab, 0.0), axis=0, keepdims=True
        )
        wvt[0:DROWS] = jnp.broadcast_to(keep, (DROWS, DH))
        wvt[DROWS : 2 * DROWS] = key
        wv_cols = jnp.transpose(write * value)

        def update(s, carry):
            column = jnp.sum(
                jnp.where(lane_q == s, wv_cols, 0.0), axis=1, keepdims=True
            )
            k_row = wvt[pl.ds(DROWS + s, 1), :]
            keep_row = wvt[pl.ds(s, 1), :]
            cv[b, s] = keep_row * cv[b, s] + column * k_row
            return carry

        lax.fori_loop(0, DROWS, update, 0)
        stores.append(pltpu.make_async_copy(cv.at[b], cell_out.at[b], wsem.at[b]))
        stores[-1].start()

        orecv[me_t] = osend[own_t]
        wait_bytes(orecv.at[pl.ds(0, TP - 1)], rsem.at[base + OUT_SEM])
        rows_sum = orecv[0].astype(F32)
        for i in range(1, TP):
            rows_sum = rows_sum + orecv[i].astype(F32)
        if b + 1 < NB:
            g[b + 1, own_t] = rows_sum.astype(BF16)
            gather_rows(b + 1, base + SEMS + ROWS_SEM)
        else:
            fin[...] = rows_sum.astype(BF16)

    for i, (src, dst) in enumerate(
        ((fin, final_out), (n1v, normer_out), (m1v, stab_out))
    ):
        stores.append(pltpu.make_async_copy(src, dst, wsem.at[NB + i]))
        stores[-1].start()
    for b in range(NB):
        base = SEMS * b
        wait_bytes(g.at[b, pl.ds(0, ROWS - TROWS)], ssem.at[base + ROWS_SEM])
        for i in range(4):
            wait_bytes(drecv.at[b, i], ssem.at[base + CORE_SEM + i])
            pieces = yrecv.at[b, i, pl.ds(0, SIDE - 1)]
            wait_bytes(pieces, ssem.at[base + CHIP_SEM + i])
        wait_bytes(trecv.at[b], ssem.at[base + CORE_SEM + 4])
        wait_bytes(tyrecv.at[b, pl.ds(0, SIDE - 1)], ssem.at[base + CHIP_SEM + 4])
        for dy in range(SIDE):
            pieces = gat.at[b, pl.ds(0, DROWS if dy == 0 else 2 * DROWS)]
            wait_bytes(pieces, ssem.at[base + GATED_SEM + dy])
        wait_bytes(outs[b][1].at[pl.ds(0, TP - 1)], ssem.at[base + OUT_SEM])
    for store in stores:
        store.wait()


def hand_on(final, cell, normer, stab, final_out, cell_out, normer_out, stab_out, *rest):
    fin, cv, n1v, m1v, sem_in, sem_out = rest
    pairs = []
    for b in range(NB):
        for i in range(PIECES):
            rows = pl.ds(i * (DROWS // PIECES), DROWS // PIECES)
            pairs.append((cell.at[b, rows], cv.at[b, rows], cell_out.at[b, rows]))
    pairs.append((final, fin, final_out))
    pairs.append((normer, n1v, normer_out))
    pairs.append((stab, m1v, stab_out))
    reads = [
        pltpu.make_async_copy(src, mid, sem_in.at[i])
        for i, (src, mid, _) in enumerate(pairs)
    ]
    writes = [
        pltpu.make_async_copy(mid, dst, sem_out.at[i])
        for i, (_, mid, dst) in enumerate(pairs)
    ]
    for read in reads:
        read.start()
    for read, write in zip(reads, writes):
        read.wait()
        write.start()
    for write in writes:
        write.wait()


def per_device(
    tokens,
    query_weight,
    key_weight,
    value_weight,
    outgate_weight,
    igate_weight,
    fgate_weight,
    norm_gain,
    head_gain,
    proj_weight,
    cell_state,
    normer_state,
    stab_state,
):
    anywhere = pl.BlockSpec(memory_space=pl.ANY)
    results = (
        jax.ShapeDtypeStruct((TROWS, COLS), BF16),
        jax.ShapeDtypeStruct((NB, DROWS, DH, DH), F32),
        jax.ShapeDtypeStruct((NB, DROWS, DH), F32),
        jax.ShapeDtypeStruct((NB, DROWS), F32),
    )
    held = pl.pallas_call(
        mega,
        out_shape=results,
        in_specs=[anywhere] * 13,
        out_specs=(anywhere,) * 4,
        scratch_shapes=[
            pltpu.VMEM((NB, ROWS, COLS), BF16),
            pltpu.VMEM((NB, COLS, QKVO), BF16),
            pltpu.VMEM((2, NB, TP, COLS), BF16),
            pltpu.VMEM((NB, TP, COLS), BF16),
            pltpu.VMEM((NB, DH, COLS), BF16),
            pltpu.VMEM((NB, COLS), F32),
            pltpu.VMEM((NB, DH), F32),
            pltpu.VMEM((NB, DROWS, DH), F32),
            pltpu.VMEM((NB, DROWS), F32),
            pltpu.VMEM((NB, DROWS, DH, DH), F32),
            pltpu.VMEM((NB, DROWS, 2 * DH, DH), BF16),
            pltpu.VMEM((ROWS, COLS), BF16),
            pltpu.VMEM((NB, 4, SIDE, DROWS, DH), F32),
            pltpu.VMEM((NB, 4, SIDE, DROWS, DH), F32),
            pltpu.VMEM((NB, 4, SIDE, DROWS, DH), F32),
            pltpu.VMEM((NB, 4, SIDE, DROWS, DH), F32),
            pltpu.VMEM((NB, 8, HALF), F32),
            pltpu.VMEM((NB, 8, HALF), F32),
            pltpu.VMEM((NB, 8, HALF), F32),
            pltpu.VMEM((NB, SIDE, 8, HALF), F32),
            pltpu.VMEM((DROWS // 8, 16, DH), BF16),
            pltpu.VMEM((2 * DROWS, DH), F32),
            pltpu.VMEM((NB, ROWS, DH), BF16),
            pltpu.VMEM((ROWS, COLS), F32),
            pltpu.VMEM((ROWS, COLS), BF16),
            pltpu.VMEM((TP, TROWS, COLS), F32),
            pltpu.VMEM((TP, TROWS, COLS), BF16),
            pltpu.VMEM((TROWS, COLS), BF16),
            pltpu.VMEM((NB, DROWS, DH), F32),
            pltpu.VMEM((NB, DROWS), F32),
            pltpu.SemaphoreType.DMA((14,)),
            pltpu.SemaphoreType.DMA((NB + 3,)),
            pltpu.SemaphoreType.DMA((SEMS * NB,)),
            pltpu.SemaphoreType.DMA((SEMS * NB,)),
        ],
        compiler_params=pltpu.CompilerParams(
            collective_id=0, has_side_effects=True, vmem_limit_bytes=60 * 10**6
        ),
        name="two_blocks",
    )(
        tokens,
        query_weight,
        key_weight,
        value_weight,
        outgate_weight,
        jnp.swapaxes(igate_weight, 1, 2),
        jnp.swapaxes(fgate_weight, 1, 2),
        norm_gain,
        head_gain,
        proj_weight,
        cell_state.reshape(NB, DROWS, DH, DH),
        normer_state.reshape(NB, DROWS, DH),
        stab_state.reshape(NB, DROWS),
    )
    moves = NB * PIECES + 3
    final_rows, cells, normers, stabs = pl.pallas_call(
        hand_on,
        out_shape=results,
        in_specs=[anywhere] * 4,
        out_specs=(anywhere,) * 4,
        scratch_shapes=[pltpu.VMEM(r.shape, r.dtype) for r in results]
        + [pltpu.SemaphoreType.DMA((moves,)), pltpu.SemaphoreType.DMA((moves,))],
        compiler_params=pltpu.CompilerParams(vmem_limit_bytes=60 * 10**6),
        name="hand_on",
    )(*held)
    return (
        final_rows,
        cells.reshape(cell_state.shape),
        normers.reshape(normer_state.shape),
        stabs.reshape(stab_state.shape),
    )


def solution(mesh):
    return jax.shard_map(
        per_device,
        mesh=mesh,
        in_specs=(
            P("tp", "dp"),
            P(None, "dp", "tp"),
            P(None, "dp", "tp"),
            P(None, "dp", "tp"),
            P(None, "dp", "tp"),
            P(),
            P(),
            P(None, "dp"),
            P(None, "tp"),
            P(None, "tp", "dp"),
            P(None, "dp", "tp", None, None),
            P(None, "dp", "tp", None),
            P(None, "dp", "tp"),
        ),
        out_specs=(
            P("tp", "dp"),
            P(None, "dp", "tp", None, None),
            P(None, "dp", "tp", None),
            P(None, "dp", "tp"),
        ),
        check_vma=False,
    )
```

```python
import functools

import jax
import jax.numpy as jnp
from jax import lax
from jax.experimental import pallas as pl
from jax.experimental.pallas import tpu as pltpu
from jax.sharding import PartitionSpec as P

D = 4096
EPSILON = 1e-06
NB = 2
TP = 16
DP = 8
ROWS = 256
DH = 128
SIDE = 4
COLS = 512
TROWS = ROWS // TP
DROWS = ROWS // DP
QKVO = 4 * DH
ROWS_SEM = 0
CORE_SEM = 4
CHIP_SEM = 8
GATED_SEM = 13
OUT_SEM = 17
SEMS = 18
ORDER = (0, 1, 4, 3, 2)
TILES = [(i * 32, 32) for i in range(4)] + [(128, 8)]
TALL = 136
GROUP = 64
NEAR_FIRST = (0, 1, 3, 2)
PIECES = 8

F32 = jnp.float32
BF16 = jnp.bfloat16


def ring_distance(step):
    return min(step, SIDE - step)


TP_STEPS = sorted(
    ((dz, dx) for dz in range(SIDE) for dx in range(SIDE) if (dz, dx) != (0, 0)),
    key=lambda s: -(ring_distance(s[0]) + ring_distance(s[1])),
)
DP_STEPS = sorted(
    ((dy, dc) for dy in range(SIDE) for dc in range(2) if (dy, dc) != (0, 0)),
    key=lambda s: -(2 * ring_distance(s[0]) + s[1]),
)


def dot_nt(a, b):
    return lax.dot_general(a, b, (((1,), (1,)), ((), ())), preferred_element_type=F32)


def mega(
    tok,
    qw,
    kw,
    vw,
    ow,
    igt,
    fgt,
    ngain,
    hgain,
    pw,
    cell,
    normer,
    stab,
    final_out,
    cell_out,
    normer_out,
    stab_out,
    g,
    w,
    gates,
    grow,
    pwv,
    ngv,
    hgv,
    n0v,
    m0v,
    cv,
    chl,
    part,
    drecv,
    yrecv,
    qs,
    wvt,
    gat,
    osend0,
    osend1,
    orecv0,
    orecv1,
    fin,
    n1v,
    m1v,
    lsem,
    wsem,
    ssem,
    rsem,
):
    me_t = lax.axis_index("tp")
    me_d = lax.axis_index("dp")
    z, x = me_t // SIDE, me_t % SIDE
    y, core = me_d // 2, me_d % 2
    tp_peers = [((z + dz) % SIDE) * SIDE + (x + dx) % SIDE for dz, dx in TP_STEPS]
    dp_peers = [((y + dy) % SIDE) * 2 + (core + dc) % 2 for dy, dc in DP_STEPS]
    partner = y * 2 + 1 - core
    own_t = pl.ds(pl.multiple_of(me_t * TROWS, TROWS), TROWS)
    own_d = pl.ds(pl.multiple_of(me_d * DROWS, DROWS), DROWS)
    own_cols = pl.ds(pl.multiple_of(me_d * COLS, COLS), COLS)

    loads = [pltpu.make_async_copy(tok, g.at[0, own_t], lsem.at[0])]
    loads.append(pltpu.make_async_copy(ngain, ngv, lsem.at[1]))
    loads.append(pltpu.make_async_copy(igt.at[:, :, own_cols], gates.at[0], lsem.at[2]))
    loads.append(pltpu.make_async_copy(fgt.at[:, :, own_cols], gates.at[1], lsem.at[3]))
    for i, src in enumerate((qw, kw, vw, ow)):
        loads.append(
            pltpu.make_async_copy(src, w.at[:, :, pl.ds(i * DH, DH)], lsem.at[4 + i])
        )
    loads.append(pltpu.make_async_copy(pw, pwv, lsem.at[8]))
    loads.append(pltpu.make_async_copy(hgain, hgv, lsem.at[9]))
    loads.append(pltpu.make_async_copy(normer, n0v, lsem.at[10]))
    loads.append(pltpu.make_async_copy(stab, m0v, lsem.at[11]))
    loads.append(pltpu.make_async_copy(cell.at[0], cv.at[0], lsem.at[12]))
    loads.append(pltpu.make_async_copy(cell.at[1], cv.at[1], lsem.at[13]))
    for load in loads:
        load.start()

    barrier = pltpu.get_barrier_semaphore()
    for t in tp_peers:
        pl.semaphore_signal(barrier, inc=1, device_id={"tp": t})
    for d in dp_peers:
        pl.semaphore_signal(barrier, inc=1, device_id={"dp": d})
    loads[0].wait()
    pl.semaphore_wait(barrier, TP + DP - 2)

    def send(src, dst, sem, axis, peer):
        pltpu.make_async_remote_copy(
            src_ref=src,
            dst_ref=dst,
            send_sem=ssem.at[sem],
            recv_sem=rsem.at[sem],
            device_id={axis: peer},
        ).start()

    def wait_bytes(ref, sem):
        pltpu.make_async_copy(ref, ref, sem).wait()

    def gather_rows(b):
        for (dz, _), t in zip(TP_STEPS, tp_peers):
            at = SEMS * b + ROWS_SEM + (SIDE - dz) % SIDE
            send(g.at[b, own_t], g.at[b, own_t], at, "tp", t)

    gather_rows(0)

    for load in loads[1:12]:
        load.wait()
    row = lax.broadcasted_iota(jnp.int32, (TP, TP), 0)
    col = lax.broadcasted_iota(jnp.int32, (TP, TP), 1)
    for b in range(NB):
        picked = jnp.zeros((TP, COLS), F32)
        for i in range(2):
            onehot = jnp.where((row == i) & (col == me_t), 1.0, 0.0).astype(BF16)
            picked = picked + jnp.dot(onehot, gates[i, b], preferred_element_type=F32)
        grow[b] = picked.astype(BF16)

    def split_cells(b):
        loads[12 + b].wait()

        def split(s, carry):
            c0 = cv[b, s]
            hi = c0.astype(BF16)
            chl[b, s, 0:DH] = hi
            chl[b, s, DH : 2 * DH] = (c0 - hi.astype(F32)).astype(BF16)
            return carry

        lax.fori_loop(0, DROWS, split, 0)

    eye = lax.broadcasted_iota(jnp.int32, (DROWS, DROWS), 0) == lax.broadcasted_iota(
        jnp.int32, (DROWS, DROWS), 1
    )
    eye_wide = lax.broadcasted_iota(
        jnp.int32, (GROUP, GROUP), 0
    ) == lax.broadcasted_iota(jnp.int32, (GROUP, GROUP), 1)
    own_lane = (
        lax.broadcasted_iota(jnp.int32, (DROWS, DH), 0) + core * DROWS
    ) == lax.broadcasted_iota(jnp.int32, (DROWS, DH), 1)
    sub8_group = lax.broadcasted_iota(jnp.int32, (8, GROUP), 0)
    sub8 = lax.broadcasted_iota(jnp.int32, (8, DH), 0)
    lane_q = lax.broadcasted_iota(jnp.int32, (DH, DROWS), 1)
    stores = []
    outs = ((osend0, orecv0), (osend1, orecv1))

    for b in range(NB):
        base = SEMS * b

        def project(k):
            dz = NEAR_FIRST[k]
            zz = (z + dz) % SIDE
            count = 3 if dz == 0 else 4
            wait_bytes(g.at[b, pl.ds(0, count * TROWS)], rsem.at[base + ROWS_SEM + dz])
            xf = g[b, pl.ds(pl.multiple_of(zz * GROUP, GROUP), GROUP)].astype(F32)
            squares = jnp.sum(xf * xf, axis=1, keepdims=True)
            scaled = (xf * ngv[pl.ds(b, 1), :]).astype(BF16)
            for i in range(2):
                two = jnp.dot(
                    scaled,
                    w[b, :, 2 * i * DH : 2 * (i + 1) * DH],
                    preferred_element_type=F32,
                )
                for n in range(2):
                    at, size = TILES[2 * i + n]
                    for c in range(2):
                        part[b, zz, c, at : at + size] = two[
                            c * DROWS : (c + 1) * DROWS, n * DH : (n + 1) * DH
                        ]
            tail = dot_nt(grow[b], scaled)
            sq_row = jnp.sum(jnp.where(eye_wide, squares, 0.0), axis=0, keepdims=True)
            tail = jnp.where(sub8_group == 2, sq_row, tail[0:8])
            tail = jnp.concatenate([tail, jnp.zeros_like(tail)], axis=1)
            for c in range(2):
                part[b, zz, c, 4 * DROWS : TALL] = tail
            sem = base + CORE_SEM + k
            send(part.at[b, zz, 1 - core], drecv.at[b, zz], sem, "dp", partner)

        def pass_on(k):
            zz = (z + NEAR_FIRST[k]) % SIDE
            wait_bytes(drecv.at[b, zz], rsem.at[base + CORE_SEM + k])
            part[b, zz, core] = part[b, zz, core] + drecv[b, zz]

            @pl.when(zz != y)
            def _():
                for i in ORDER:
                    rows = pl.ds(*TILES[i])
                    src, dst = part.at[b, zz, core, rows], yrecv.at[b, y, rows]
                    send(src, dst, base + CHIP_SEM + i, "dp", zz * 2 + core)

        for k in range(SIDE):
            project(k)
            if k > 0:
                pass_on(k - 1)
        pass_on(SIDE - 1)
        if b == 0:
            split_cells(0)

        def arrived(i):
            at, size = TILES[i]
            wait_bytes(
                yrecv.at[b, 0, pl.ds(0, 3 * size)], rsem.at[base + CHIP_SEM + i]
            )
            total = part[b, y, core, at : at + size]
            for dy in range(1, SIDE):
                total = total + yrecv[b, (y + dy) % SIDE, at : at + size]
            return total

        query = arrived(0)
        q_hi = query.astype(BF16).astype(F32)
        q_lo = query - q_hi
        groups = []
        for j in range(DROWS // 8):
            rows = slice(8 * j, 8 * j + 8)
            qs[j] = jnp.concatenate([q_hi[rows], q_lo[rows]], axis=0).astype(BF16)
        for j in range(DROWS // 8):
            acc = jnp.zeros((8, DH), F32)
            for i in range(8):
                r = dot_nt(qs[j], chl[b, 8 * j + i])
                r = r[0:8, 0:DH] + (r[8:16, 0:DH] + r[0:8, DH : 2 * DH])
                acc = jnp.where(sub8 == i, r, acc)
            groups.append(acc)
        old_read = jnp.concatenate(groups, axis=0)

        key = arrived(1)
        tail = arrived(4)

        def column(i):
            return jnp.sum(
                jnp.where(own_lane, tail[i : i + 1], 0.0), axis=1, keepdims=True
            )

        inv_rms = lax.rsqrt(column(2) * (1.0 / D) + EPSILON)
        query = query * inv_rms
        old_read = old_read * inv_rms
        key = key * (inv_rms * DH**-0.5)
        igate = column(0) * inv_rms
        fpre = column(1) * inv_rms
        forget = jnp.minimum(fpre, 0.0) - jnp.log1p(jnp.exp(-jnp.abs(fpre)))
        prev = jnp.sum(jnp.where(eye, m0v[pl.ds(b, 1), :], 0.0), axis=1, keepdims=True)
        new_stab = jnp.maximum(forget + prev, igate)
        keep = jnp.exp(forget + prev - new_stab)
        write = jnp.exp(igate - new_stab)
        new_normer = keep * n0v[b] + write * key
        key_query = jnp.sum(key * query, axis=1, keepdims=True)
        denom = jnp.maximum(
            jnp.abs(jnp.sum(new_normer * query, axis=1, keepdims=True)), 1.0
        )
        outgate = arrived(3) * inv_rms
        scale = hgv[pl.ds(b, 1), :] / (1.0 + jnp.exp(-outgate))
        value = arrived(2) * inv_rms
        numer = keep * old_read + (write * key_query) * value
        readout = numer / denom
        normed = readout * lax.rsqrt(
            jnp.mean(readout * readout, axis=1, keepdims=True) + EPSILON
        )
        gat[b, own_d] = (normed * scale).astype(BF16)
        for d in dp_peers:
            send(gat.at[b, own_d], gat.at[b, own_d], base + GATED_SEM + y, "dp", d)

        osend, orecv = outs[b]
        for dz in NEAR_FIRST:
            yy = (z + dz) % SIDE

            @pl.when(yy == y)
            def _():
                wait_bytes(gat.at[b, pl.ds(0, DROWS)], rsem.at[base + GATED_SEM + yy])

            @pl.when(yy != y)
            def _():
                wait_bytes(gat.at[b, pl.ds(0, GROUP)], rsem.at[base + GATED_SEM + yy])

            rows = pl.ds(pl.multiple_of(yy * GROUP, GROUP), GROUP)
            osend[rows] = jnp.dot(
                gat[b, rows], pwv[b], preferred_element_type=F32
            ).astype(osend.dtype)
            for dx in (2, 1, 3, 0):
                if (dz, dx) == (0, 0):
                    continue
                t = yy * SIDE + (x + dx) % SIDE
                src = osend.at[pl.ds(pl.multiple_of(t * TROWS, TROWS), TROWS)]
                send(src, orecv.at[me_t], base + OUT_SEM, "tp", t)

        n1v[b] = new_normer
        m1v[pl.ds(b, 1), :] = jnp.sum(
            jnp.where(eye, new_stab, 0.0), axis=0, keepdims=True
        )
        wvt[0:DROWS] = jnp.broadcast_to(keep, (DROWS, DH))
        wvt[DROWS : 2 * DROWS] = key
        wv_cols = jnp.transpose(write * value)

        def update(s, carry):
            column = jnp.sum(
                jnp.where(lane_q == s, wv_cols, 0.0), axis=1, keepdims=True
            )
            k_row = wvt[pl.ds(DROWS + s, 1), :]
            keep_row = wvt[pl.ds(s, 1), :]
            cv[b, s] = keep_row * cv[b, s] + column * k_row
            return carry

        lax.fori_loop(0, DROWS, update, 0)
        stores.append(pltpu.make_async_copy(cv.at[b], cell_out.at[b], wsem.at[b]))
        stores[-1].start()
        if b == 0:
            split_cells(1)

        orecv[me_t] = osend[own_t]
        wait_bytes(orecv.at[pl.ds(0, TP - 1)], rsem.at[base + OUT_SEM])
        rows_sum = orecv[0].astype(F32)
        for i in range(1, TP):
            rows_sum = rows_sum + orecv[i].astype(F32)
        if b + 1 < NB:
            g[b + 1, own_t] = rows_sum.astype(BF16)
            gather_rows(b + 1)
        else:
            fin[...] = rows_sum.astype(BF16)

    for i, (src, dst) in enumerate(
        ((fin, final_out), (n1v, normer_out), (m1v, stab_out))
    ):
        stores.append(pltpu.make_async_copy(src, dst, wsem.at[NB + i]))
        stores[-1].start()
    for b in range(NB):
        base = SEMS * b
        for k in range(SIDE):
            count = 3 if k == 0 else 4
            wait_bytes(g.at[b, pl.ds(0, count * TROWS)], ssem.at[base + ROWS_SEM + k])
            wait_bytes(drecv.at[b, k], ssem.at[base + CORE_SEM + k])
        for i in range(5):
            pieces = yrecv.at[b, 0, pl.ds(0, 3 * TILES[i][1])]
            wait_bytes(pieces, ssem.at[base + CHIP_SEM + i])
        pieces = gat.at[b, pl.ds(0, (DP - 1) * DROWS)]
        wait_bytes(pieces, ssem.at[base + GATED_SEM + y])
        wait_bytes(outs[b][1].at[pl.ds(0, TP - 1)], ssem.at[base + OUT_SEM])
    for store in stores:
        store.wait()


def hand_on(final, cell, normer, stab, final_out, cell_out, normer_out, stab_out, *rest):
    fin, cv, n1v, m1v, sem_in, sem_out = rest
    pairs = []
    for b in range(NB):
        for i in range(PIECES):
            rows = pl.ds(i * (DROWS // PIECES), DROWS // PIECES)
            pairs.append((cell.at[b, rows], cv.at[b, rows], cell_out.at[b, rows]))
    pairs.append((final, fin, final_out))
    pairs.append((normer, n1v, normer_out))
    pairs.append((stab, m1v, stab_out))
    reads = [
        pltpu.make_async_copy(src, mid, sem_in.at[i])
        for i, (src, mid, _) in enumerate(pairs)
    ]
    writes = [
        pltpu.make_async_copy(mid, dst, sem_out.at[i])
        for i, (_, mid, dst) in enumerate(pairs)
    ]
    for read in reads:
        read.start()
    for read, write in zip(reads, writes):
        read.wait()
        write.start()
    for write in writes:
        write.wait()


def per_device(
    tokens,
    query_weight,
    key_weight,
    value_weight,
    outgate_weight,
    igate_weight,
    fgate_weight,
    norm_gain,
    head_gain,
    proj_weight,
    cell_state,
    normer_state,
    stab_state,
):
    anywhere = pl.BlockSpec(memory_space=pl.ANY)
    results = (
        jax.ShapeDtypeStruct((TROWS, COLS), BF16),
        jax.ShapeDtypeStruct((NB, DROWS, DH, DH), F32),
        jax.ShapeDtypeStruct((NB, DROWS, DH), F32),
        jax.ShapeDtypeStruct((NB, DROWS), F32),
    )
    held = pl.pallas_call(
        mega,
        out_shape=results,
        in_specs=[anywhere] * 13,
        out_specs=(anywhere,) * 4,
        scratch_shapes=[
            pltpu.VMEM((NB, ROWS, COLS), BF16),
            pltpu.VMEM((NB, COLS, QKVO), BF16),
            pltpu.VMEM((2, NB, TP, COLS), BF16),
            pltpu.VMEM((NB, TP, COLS), BF16),
            pltpu.VMEM((NB, DH, COLS), BF16),
            pltpu.VMEM((NB, COLS), F32),
            pltpu.VMEM((NB, DH), F32),
            pltpu.VMEM((NB, DROWS, DH), F32),
            pltpu.VMEM((NB, DROWS), F32),
            pltpu.VMEM((NB, DROWS, DH, DH), F32),
            pltpu.VMEM((NB, DROWS, 2 * DH, DH), BF16),
            pltpu.VMEM((NB, SIDE, 2, TALL, DH), F32),
            pltpu.VMEM((NB, SIDE, TALL, DH), F32),
            pltpu.VMEM((NB, SIDE, TALL, DH), F32),
            pltpu.VMEM((DROWS // 8, 16, DH), BF16),
            pltpu.VMEM((2 * DROWS, DH), F32),
            pltpu.VMEM((NB, ROWS, DH), BF16),
            pltpu.VMEM((ROWS, COLS), F32),
            pltpu.VMEM((ROWS, COLS), BF16),
            pltpu.VMEM((TP, TROWS, COLS), F32),
            pltpu.VMEM((TP, TROWS, COLS), BF16),
            pltpu.VMEM((TROWS, COLS), BF16),
            pltpu.VMEM((NB, DROWS, DH), F32),
            pltpu.VMEM((NB, DROWS), F32),
            pltpu.SemaphoreType.DMA((14,)),
            pltpu.SemaphoreType.DMA((NB + 3,)),
            pltpu.SemaphoreType.DMA((SEMS * NB,)),
            pltpu.SemaphoreType.DMA((SEMS * NB,)),
        ],
        compiler_params=pltpu.CompilerParams(
            collective_id=0, has_side_effects=True, vmem_limit_bytes=60 * 10**6
        ),
        name="two_blocks",
    )(
        tokens,
        query_weight,
        key_weight,
        value_weight,
        outgate_weight,
        jnp.swapaxes(igate_weight, 1, 2),
        jnp.swapaxes(fgate_weight, 1, 2),
        norm_gain,
        head_gain,
        proj_weight,
        cell_state.reshape(NB, DROWS, DH, DH),
        normer_state.reshape(NB, DROWS, DH),
        stab_state.reshape(NB, DROWS),
    )
    moves = NB * PIECES + 3
    final_rows, cells, normers, stabs = pl.pallas_call(
        hand_on,
        out_shape=results,
        in_specs=[anywhere] * 4,
        out_specs=(anywhere,) * 4,
        scratch_shapes=[pltpu.VMEM(r.shape, r.dtype) for r in results]
        + [pltpu.SemaphoreType.DMA((moves,)), pltpu.SemaphoreType.DMA((moves,))],
        compiler_params=pltpu.CompilerParams(vmem_limit_bytes=60 * 10**6),
        name="hand_on",
    )(*held)
    return (
        final_rows,
        cells.reshape(cell_state.shape),
        normers.reshape(normer_state.shape),
        stabs.reshape(stab_state.shape),
    )


def solution(mesh):
    return jax.shard_map(
        per_device,
        mesh=mesh,
        in_specs=(
            P("tp", "dp"),
            P(None, "dp", "tp"),
            P(None, "dp", "tp"),
            P(None, "dp", "tp"),
            P(None, "dp", "tp"),
            P(),
            P(),
            P(None, "dp"),
            P(None, "tp"),
            P(None, "tp", "dp"),
            P(None, "dp", "tp", None, None),
            P(None, "dp", "tp", None),
            P(None, "dp", "tp"),
        ),
        out_specs=(
            P("tp", "dp"),
            P(None, "dp", "tp", None, None),
            P(None, "dp", "tp", None),
            P(None, "dp", "tp"),
        ),
        check_vma=False,
    )
```

```python
import functools

import jax
import jax.numpy as jnp
from jax import lax
from jax.experimental import pallas as pl
from jax.experimental.pallas import tpu as pltpu
from jax.sharding import PartitionSpec as P

D = 4096
EPSILON = 1e-06
NB = 2
TP = 16
DP = 8
ROWS = 256
DH = 128
SIDE = 4
COLS = 512
TROWS = ROWS // TP
DROWS = ROWS // DP
QKVO = 4 * DH
ROWS_SEM = 0
CORE_SEM = 4
CHIP_SEM = 8
GATED_SEM = 13
OUT_SEM = 17
WEIGHT_SEM = 18
SEMS = 19
ORDER = (0, 1, 4, 3, 2)
TILES = [(i * 32, 32) for i in range(4)] + [(128, 8)]
TALL = 136
GROUP = 64
NEAR_FIRST = (0, 1, 3, 2)
PIECES = 8

F32 = jnp.float32
BF16 = jnp.bfloat16


def ring_distance(step):
    return min(step, SIDE - step)


TP_STEPS = sorted(
    ((dz, dx) for dz in range(SIDE) for dx in range(SIDE) if (dz, dx) != (0, 0)),
    key=lambda s: (-ring_distance(s[0]), -ring_distance(s[1])),
)
DP_STEPS = sorted(
    ((dy, dc) for dy in range(SIDE) for dc in range(2) if (dy, dc) != (0, 0)),
    key=lambda s: -(2 * ring_distance(s[0]) + s[1]),
)


def dot_nt(a, b):
    return lax.dot_general(a, b, (((1,), (1,)), ((), ())), preferred_element_type=F32)


def mega(
    tok,
    qw,
    kw,
    vw,
    ow,
    igt,
    fgt,
    ngain,
    hgain,
    pw,
    cell,
    normer,
    stab,
    final_out,
    cell_out,
    normer_out,
    stab_out,
    g,
    w,
    gates,
    grow,
    pwv,
    ngv,
    hgv,
    n0v,
    m0v,
    cv,
    chl,
    part,
    drecv,
    yrecv,
    qs,
    wvt,
    gsend,
    gat,
    osend,
    orecv,
    fin,
    n1v,
    m1v,
    lsem,
    wsem,
    ssem,
    rsem,
):
    me_t = lax.axis_index("tp")
    me_d = lax.axis_index("dp")
    z, x = me_t // SIDE, me_t % SIDE
    y, core = me_d // 2, me_d % 2
    tp_peers = [((z + dz) % SIDE) * SIDE + (x + dx) % SIDE for dz, dx in TP_STEPS]
    dp_peers = [((y + dy) % SIDE) * 2 + (core + dc) % 2 for dy, dc in DP_STEPS]
    partner = y * 2 + 1 - core
    own_t = pl.ds(pl.multiple_of(me_t * TROWS, TROWS), TROWS)
    own_cols = pl.ds(pl.multiple_of(me_d * COLS, COLS), COLS)

    loads = [pltpu.make_async_copy(tok, g.at[0, own_t], lsem.at[0])]
    loads.append(pltpu.make_async_copy(ngain, ngv, lsem.at[1]))
    loads.append(pltpu.make_async_copy(igt.at[:, :, own_cols], gates.at[0], lsem.at[2]))
    loads.append(pltpu.make_async_copy(fgt.at[:, :, own_cols], gates.at[1], lsem.at[3]))
    for i, src in enumerate((qw, kw, vw, ow)):
        loads.append(
            pltpu.make_async_copy(src, w.at[:, :, pl.ds(i * DH, DH)], lsem.at[4 + i])
        )
    loads.append(pltpu.make_async_copy(pw.at[0], pwv.at[0, z], lsem.at[8]))
    loads.append(pltpu.make_async_copy(hgain, hgv, lsem.at[9]))
    loads.append(pltpu.make_async_copy(normer, n0v, lsem.at[10]))
    loads.append(pltpu.make_async_copy(stab, m0v, lsem.at[11]))
    loads.append(pltpu.make_async_copy(pw.at[1], pwv.at[1, z], lsem.at[14]))
    loads.append(pltpu.make_async_copy(cell.at[0], cv.at[0], lsem.at[12]))
    loads.append(pltpu.make_async_copy(cell.at[1], cv.at[1], lsem.at[13]))
    loads[0].start()
    barrier = pltpu.get_barrier_semaphore()
    for t in tp_peers:
        pl.semaphore_signal(barrier, inc=1, device_id={"tp": t})
    for d in dp_peers:
        pl.semaphore_signal(barrier, inc=1, device_id={"dp": d})
    for load in loads[1:]:
        load.start()
    loads[0].wait()
    pl.semaphore_wait(barrier, TP + DP - 2)

    def send(src, dst, sem, axis, peer):
        pltpu.make_async_remote_copy(
            src_ref=src,
            dst_ref=dst,
            send_sem=ssem.at[sem],
            recv_sem=rsem.at[sem],
            device_id={axis: peer},
        ).start()

    def wait_bytes(ref, sem):
        pltpu.make_async_copy(ref, ref, sem).wait()

    def gather_rows(b):
        for (dz, _), t in zip(TP_STEPS, tp_peers):
            at = SEMS * b + ROWS_SEM + (SIDE - dz) % SIDE
            send(g.at[b, own_t], g.at[b, own_t], at, "tp", t)

    gather_rows(0)

    for load in loads[1:13]:
        load.wait()
    row = lax.broadcasted_iota(jnp.int32, (TP, TP), 0)
    col = lax.broadcasted_iota(jnp.int32, (TP, TP), 1)
    for b in range(NB):
        picked = jnp.zeros((TP, COLS), F32)
        for i in range(2):
            onehot = jnp.where((row == i) & (col == me_t), 1.0, 0.0).astype(BF16)
            picked = picked + jnp.dot(onehot, gates[i, b], preferred_element_type=F32)
        grow[b] = picked.astype(BF16)

    def split_cells(b):
        loads[13 + b].wait()

        def split(s, carry):
            c0 = cv[b, s]
            hi = c0.astype(BF16)
            chl[b, s, 0:DH] = hi
            chl[b, s, DH : 2 * DH] = (c0 - hi.astype(F32)).astype(BF16)
            return carry

        lax.fori_loop(0, DROWS, split, 0)

    eye = lax.broadcasted_iota(jnp.int32, (DROWS, DROWS), 0) == lax.broadcasted_iota(
        jnp.int32, (DROWS, DROWS), 1
    )
    eye_wide = lax.broadcasted_iota(
        jnp.int32, (GROUP, GROUP), 0
    ) == lax.broadcasted_iota(jnp.int32, (GROUP, GROUP), 1)
    own_lane = (
        lax.broadcasted_iota(jnp.int32, (DROWS, DH), 0) + core * DROWS
    ) == lax.broadcasted_iota(jnp.int32, (DROWS, DH), 1)
    sub8_group = lax.broadcasted_iota(jnp.int32, (8, GROUP), 0)
    sub8 = lax.broadcasted_iota(jnp.int32, (8, DH), 0)
    lane_q = lax.broadcasted_iota(jnp.int32, (DH, DROWS), 1)
    stores = []

    for b in range(NB):
        base = SEMS * b

        def project(k):
            dz = NEAR_FIRST[k]
            zz = (z + dz) % SIDE
            count = 3 if dz == 0 else 4
            wait_bytes(g.at[b, pl.ds(0, count * TROWS)], rsem.at[base + ROWS_SEM + dz])
            xf = g[b, pl.ds(pl.multiple_of(zz * GROUP, GROUP), GROUP)].astype(F32)
            squares = jnp.sum(xf * xf, axis=1, keepdims=True)
            scaled = (xf * ngv[pl.ds(b, 1), :]).astype(BF16)
            for i in range(2):
                two = jnp.dot(
                    scaled,
                    w[b, :, 2 * i * DH : 2 * (i + 1) * DH],
                    preferred_element_type=F32,
                )
                for n in range(2):
                    at, size = TILES[2 * i + n]
                    for c in range(2):
                        part[b, zz, c, at : at + size] = two[
                            c * DROWS : (c + 1) * DROWS, n * DH : (n + 1) * DH
                        ]
            tail = dot_nt(grow[b], scaled)
            sq_row = jnp.sum(jnp.where(eye_wide, squares, 0.0), axis=0, keepdims=True)
            tail = jnp.where(sub8_group == 2, sq_row, tail[0:8])
            tail = jnp.concatenate([tail, jnp.zeros_like(tail)], axis=1)
            for c in range(2):
                part[b, zz, c, 4 * DROWS : TALL] = tail
            sem = base + CORE_SEM + k
            send(part.at[b, zz, 1 - core], drecv.at[b, zz], sem, "dp", partner)

        def pass_on(k):
            zz = (z + NEAR_FIRST[k]) % SIDE
            wait_bytes(drecv.at[b, zz], rsem.at[base + CORE_SEM + k])
            part[b, zz, core] = part[b, zz, core] + drecv[b, zz]

            @pl.when(zz != y)
            def _():
                for i in ORDER:
                    rows = pl.ds(*TILES[i])
                    src, dst = part.at[b, zz, core, rows], yrecv.at[b, y, rows]
                    send(src, dst, base + CHIP_SEM + i, "dp", zz * 2 + core)

        for k in range(SIDE):
            project(k)
            if k > 0:
                pass_on(k - 1)
        for dz in (2, 1, 3):
            t = (z + dz) % SIDE * SIDE + x
            send(pwv.at[b, z], pwv.at[b, z], base + WEIGHT_SEM, "tp", t)
        pass_on(SIDE - 1)
        if b == 0:
            split_cells(0)

        def arrived(i):
            at, size = TILES[i]
            wait_bytes(
                yrecv.at[b, 0, pl.ds(0, 3 * size)], rsem.at[base + CHIP_SEM + i]
            )
            total = part[b, y, core, at : at + size]
            for dy in range(1, SIDE):
                total = total + yrecv[b, (y + dy) % SIDE, at : at + size]
            return total

        query = arrived(0)
        q_hi = query.astype(BF16).astype(F32)
        q_lo = query - q_hi
        groups = []
        for j in range(DROWS // 8):
            rows = slice(8 * j, 8 * j + 8)
            qs[j] = jnp.concatenate([q_hi[rows], q_lo[rows]], axis=0).astype(BF16)
        for j in range(DROWS // 8):
            acc = jnp.zeros((8, DH), F32)
            for i in range(8):
                r = dot_nt(qs[j], chl[b, 8 * j + i])
                r = r[0:8, 0:DH] + (r[8:16, 0:DH] + r[0:8, DH : 2 * DH])
                acc = jnp.where(sub8 == i, r, acc)
            groups.append(acc)
        old_read = jnp.concatenate(groups, axis=0)

        key = arrived(1)
        tail = arrived(4)

        def column(i):
            return jnp.sum(
                jnp.where(own_lane, tail[i : i + 1], 0.0), axis=1, keepdims=True
            )

        inv_rms = lax.rsqrt(column(2) * (1.0 / D) + EPSILON)
        query = query * inv_rms
        old_read = old_read * inv_rms
        key = key * (inv_rms * DH**-0.5)
        igate = column(0) * inv_rms
        fpre = column(1) * inv_rms
        forget = jnp.minimum(fpre, 0.0) - jnp.log1p(jnp.exp(-jnp.abs(fpre)))
        prev = jnp.sum(jnp.where(eye, m0v[pl.ds(b, 1), :], 0.0), axis=1, keepdims=True)
        new_stab = jnp.maximum(forget + prev, igate)
        keep = jnp.exp(forget + prev - new_stab)
        write = jnp.exp(igate - new_stab)
        new_normer = keep * n0v[b] + write * key
        key_query = jnp.sum(key * query, axis=1, keepdims=True)
        denom = jnp.maximum(
            jnp.abs(jnp.sum(new_normer * query, axis=1, keepdims=True)), 1.0
        )
        outgate = arrived(3) * inv_rms
        scale = hgv[pl.ds(b, 1), :] / (1.0 + jnp.exp(-outgate))
        value = arrived(2) * inv_rms
        numer = keep * old_read + (write * key_query) * value
        readout = numer / denom
        normed = readout * lax.rsqrt(
            jnp.mean(readout * readout, axis=1, keepdims=True) + EPSILON
        )
        gsend[b] = (normed * scale).astype(BF16)

        def give_gated(dy, dc):
            pltpu.make_async_remote_copy(
                src_ref=gsend.at[b],
                dst_ref=gat.at[b, 2 * z + core],
                send_sem=ssem.at[base + GATED_SEM],
                recv_sem=rsem.at[base + GATED_SEM + (z - y + SIDE) % SIDE],
                device_id={
                    "tp": y * SIDE + x,
                    "dp": (y + dy) % SIDE * 2 + (core + dc) % 2,
                },
            ).start()

        for dy, dc in DP_STEPS:
            give_gated(dy, dc)

        @pl.when(y != z)
        def _():
            give_gated(0, 0)

        @pl.when(y == z)
        def _():
            gat[b, 2 * z + core] = gsend[b]

        n1v[b] = new_normer
        m1v[pl.ds(b, 1), :] = jnp.sum(
            jnp.where(eye, new_stab, 0.0), axis=0, keepdims=True
        )
        wvt[0:DROWS] = jnp.broadcast_to(keep, (DROWS, DH))
        wvt[DROWS : 2 * DROWS] = key
        wv_cols = jnp.transpose(write * value)

        def update(s, carry):
            column = jnp.sum(
                jnp.where(lane_q == s, wv_cols, 0.0), axis=1, keepdims=True
            )
            k_row = wvt[pl.ds(DROWS + s, 1), :]
            keep_row = wvt[pl.ds(s, 1), :]
            cv[b, s] = keep_row * cv[b, s] + column * k_row
            return carry

        lax.fori_loop(0, DROWS, update, 0)
        stores.append(pltpu.make_async_copy(cv.at[b], cell_out.at[b], wsem.at[b]))
        stores[-1].start()
        for dz in NEAR_FIRST:
            zz = (z + dz) % SIDE
            at = rsem.at[base + GATED_SEM + dz]
            if dz == 0:

                @pl.when(y == z)
                def _():
                    wait_bytes(gat.at[b, pl.ds(0, 1)], at)

                @pl.when(y != z)
                def _():
                    wait_bytes(gat.at[b, pl.ds(0, 2)], at)

                partial = jnp.zeros((GROUP, COLS), F32)
            else:
                wait_bytes(gat.at[b, pl.ds(0, 2)], at)
            if dz == 1:
                pieces = pwv.at[b, pl.ds(0, SIDE - 1)]
                wait_bytes(pieces, rsem.at[base + WEIGHT_SEM])
            rows = jnp.concatenate([gat[b, 2 * zz], gat[b, 2 * zz + 1]], axis=0)
            partial = partial + jnp.dot(
                rows, pwv[b, zz], preferred_element_type=F32
            )
        osend[b] = partial

        for dx in (2, 1, 3):
            xx = (x + dx) % SIDE
            rows = pl.ds(pl.multiple_of(xx * TROWS, TROWS), TROWS)
            t = z * SIDE + xx
            send(osend.at[b, rows], orecv.at[b, x], base + OUT_SEM, "tp", t)
        if b == 0:
            split_cells(1)
        rows = pl.ds(pl.multiple_of(x * TROWS, TROWS), TROWS)
        orecv[b, x] = osend[b, rows]
        wait_bytes(orecv.at[b, pl.ds(0, SIDE - 1)], rsem.at[base + OUT_SEM])
        rows_sum = orecv[b, 0] + orecv[b, 1] + (orecv[b, 2] + orecv[b, 3])
        if b + 1 < NB:
            g[b + 1, own_t] = rows_sum.astype(BF16)
            gather_rows(b + 1)
        else:
            fin[...] = rows_sum.astype(BF16)

    for i, (src, dst) in enumerate(
        ((fin, final_out), (n1v, normer_out), (m1v, stab_out))
    ):
        stores.append(pltpu.make_async_copy(src, dst, wsem.at[NB + i]))
        stores[-1].start()
    for b in range(NB):
        base = SEMS * b
        for k in range(SIDE):
            count = 3 if k == 0 else 4
            wait_bytes(g.at[b, pl.ds(0, count * TROWS)], ssem.at[base + ROWS_SEM + k])
            wait_bytes(drecv.at[b, k], ssem.at[base + CORE_SEM + k])
        for i in range(5):
            pieces = yrecv.at[b, 0, pl.ds(0, 3 * TILES[i][1])]
            wait_bytes(pieces, ssem.at[base + CHIP_SEM + i])

        @pl.when(y == z)
        def _():
            wait_bytes(gat.at[b, pl.ds(0, DP - 1)], ssem.at[base + GATED_SEM])

        @pl.when(y != z)
        def _():
            wait_bytes(gat.at[b], ssem.at[base + GATED_SEM])

        wait_bytes(orecv.at[b, pl.ds(0, SIDE - 1)], ssem.at[base + OUT_SEM])
        wait_bytes(pwv.at[b, pl.ds(0, SIDE - 1)], ssem.at[base + WEIGHT_SEM])
    for store in stores:
        store.wait()


def hand_on(final, cell, normer, stab, final_out, cell_out, normer_out, stab_out, *rest):
    fin, cv, n1v, m1v, sem_in, sem_out = rest
    pairs = []
    for b in range(NB):
        for i in range(PIECES):
            rows = pl.ds(i * (DROWS // PIECES), DROWS // PIECES)
            pairs.append((cell.at[b, rows], cv.at[b, rows], cell_out.at[b, rows]))
    pairs.append((final, fin, final_out))
    pairs.append((normer, n1v, normer_out))
    pairs.append((stab, m1v, stab_out))
    reads = [
        pltpu.make_async_copy(src, mid, sem_in.at[i])
        for i, (src, mid, _) in enumerate(pairs)
    ]
    writes = [
        pltpu.make_async_copy(mid, dst, sem_out.at[i])
        for i, (_, mid, dst) in enumerate(pairs)
    ]
    for read in reads:
        read.start()
    for read, write in zip(reads, writes):
        read.wait()
        write.start()
    for write in writes:
        write.wait()


def per_device(
    tokens,
    query_weight,
    key_weight,
    value_weight,
    outgate_weight,
    igate_weight,
    fgate_weight,
    norm_gain,
    head_gain,
    proj_weight,
    cell_state,
    normer_state,
    stab_state,
):
    anywhere = pl.BlockSpec(memory_space=pl.ANY)
    results = (
        jax.ShapeDtypeStruct((TROWS, COLS), BF16),
        jax.ShapeDtypeStruct((NB, DROWS, DH, DH), F32),
        jax.ShapeDtypeStruct((NB, DROWS, DH), F32),
        jax.ShapeDtypeStruct((NB, DROWS), F32),
    )
    held = pl.pallas_call(
        mega,
        out_shape=results,
        in_specs=[anywhere] * 13,
        out_specs=(anywhere,) * 4,
        scratch_shapes=[
            pltpu.VMEM((NB, ROWS, COLS), BF16),
            pltpu.VMEM((NB, COLS, QKVO), BF16),
            pltpu.VMEM((2, NB, TP, COLS), BF16),
            pltpu.VMEM((NB, TP, COLS), BF16),
            pltpu.VMEM((NB, SIDE, DH, COLS), BF16),
            pltpu.VMEM((NB, COLS), F32),
            pltpu.VMEM((NB, DH), F32),
            pltpu.VMEM((NB, DROWS, DH), F32),
            pltpu.VMEM((NB, DROWS), F32),
            pltpu.VMEM((NB, DROWS, DH, DH), F32),
            pltpu.VMEM((NB, DROWS, 2 * DH, DH), BF16),
            pltpu.VMEM((NB, SIDE, 2, TALL, DH), F32),
            pltpu.VMEM((NB, SIDE, TALL, DH), F32),
            pltpu.VMEM((NB, SIDE, TALL, DH), F32),
            pltpu.VMEM((DROWS // 8, 16, DH), BF16),
            pltpu.VMEM((2 * DROWS, DH), F32),
            pltpu.VMEM((NB, DROWS, DH), BF16),
            pltpu.VMEM((NB, DP, DROWS, DH), BF16),
            pltpu.VMEM((NB, GROUP, COLS), F32),
            pltpu.VMEM((NB, SIDE, TROWS, COLS), F32),
            pltpu.VMEM((TROWS, COLS), BF16),
            pltpu.VMEM((NB, DROWS, DH), F32),
            pltpu.VMEM((NB, DROWS), F32),
            pltpu.SemaphoreType.DMA((15,)),
            pltpu.SemaphoreType.DMA((NB + 3,)),
            pltpu.SemaphoreType.DMA((SEMS * NB,)),
            pltpu.SemaphoreType.DMA((SEMS * NB,)),
        ],
        compiler_params=pltpu.CompilerParams(
            collective_id=0, has_side_effects=True, vmem_limit_bytes=60 * 10**6
        ),
        name="two_blocks",
    )(
        tokens,
        query_weight,
        key_weight,
        value_weight,
        outgate_weight,
        jnp.swapaxes(igate_weight, 1, 2),
        jnp.swapaxes(fgate_weight, 1, 2),
        norm_gain,
        head_gain,
        proj_weight,
        cell_state.reshape(NB, DROWS, DH, DH),
        normer_state.reshape(NB, DROWS, DH),
        stab_state.reshape(NB, DROWS),
    )
    moves = NB * PIECES + 3
    final_rows, cells, normers, stabs = pl.pallas_call(
        hand_on,
        out_shape=results,
        in_specs=[anywhere] * 4,
        out_specs=(anywhere,) * 4,
        scratch_shapes=[pltpu.VMEM(r.shape, r.dtype) for r in results]
        + [pltpu.SemaphoreType.DMA((moves,)), pltpu.SemaphoreType.DMA((moves,))],
        compiler_params=pltpu.CompilerParams(vmem_limit_bytes=60 * 10**6),
        name="hand_on",
    )(*held)
    return (
        final_rows,
        cells.reshape(cell_state.shape),
        normers.reshape(normer_state.shape),
        stabs.reshape(stab_state.shape),
    )


def solution(mesh):
    return jax.shard_map(
        per_device,
        mesh=mesh,
        in_specs=(
            P("tp", "dp"),
            P(None, "dp", "tp"),
            P(None, "dp", "tp"),
            P(None, "dp", "tp"),
            P(None, "dp", "tp"),
            P(),
            P(),
            P(None, "dp"),
            P(None, "tp"),
            P(None, "tp", "dp"),
            P(None, "dp", "tp", None, None),
            P(None, "dp", "tp", None),
            P(None, "dp", "tp"),
        ),
        out_specs=(
            P("tp", "dp"),
            P(None, "dp", "tp", None, None),
            P(None, "dp", "tp", None),
            P(None, "dp", "tp"),
        ),
        check_vma=False,
    )
```
